32 devices in a mesh: fs: 4 (over z), rep: 4 (over y, x), tp: 2 (over core).
Axes of the slice: x: 2, y: 2, z: 4, core: 2. Of those that a mesh axis runs over, the one named last changes fastest.
Arguments:
- query_input: bfloat16 [16384, 4096], P(('fs', 'rep')), may hold values from -6 to 6
- query_cotangent: bfloat16 [16384, 1024], P(('fs', 'rep'), 'tp'), may hold values from -0.046875 to 0.046875
- branch_output: bfloat16 [16384, 2048], P(('fs', 'rep')), may hold values from -6 to 6
- layer_cotangent: bfloat16 [16384, 4096], P(('fs', 'rep'), 'tp'), may hold values from -0.046875 to 0.046875
- query_weight: float32 [4096, 1024], P(('rep', 'fs'), 'tp'), may hold values from -0.09375 to 0.09375
- output_weight: float32 [2048, 4096], P(('rep', 'fs'), 'tp'), may hold values from -0.125 to 0.125
- query_basis: bfloat16 [4096, 512], P(('rep', 'fs')), may hold values from -0.09375 to 0.09375
- output_basis: bfloat16 [2048, 512], P(('rep', 'fs')), may hold values from -0.125 to 0.125
- query_first: float32 [512, 1024], P(('rep', 'fs'), 'tp'), may hold values from -20 to 20
- query_second: float32 [512, 1024], P(('rep', 'fs'), 'tp'), may hold values from 0.25 to 2
- output_first: float32 [512, 4096], P(('rep', 'fs'), 'tp'), may hold values from -20 to 20
- output_second: float32 [512, 4096], P(('rep', 'fs'), 'tp'), may hold values from 0.25 to 2
Outputs:
- query_update: float32 [4096, 1024], P(('rep', 'fs'), 'tp')
- output_update: float32 [2048, 4096], P(('rep', 'fs'), 'tp')
- query_first_next: float32 [512, 1024], P(('rep', 'fs'), 'tp')
- query_second_next: float32 [512, 1024], P(('rep', 'fs'), 'tp')
- output_first_next: float32 [512, 4096], P(('rep', 'fs'), 'tp')
- output_second_next: float32 [512, 4096], P(('rep', 'fs'), 'tp')
- query_copy: bfloat16 [4096, 1024], P('rep', 'tp')
- output_copy: bfloat16 [2048, 4096], P('rep', 'tp')
The draws below stay inside these ranges and needn't reach their ends.
All inputs are finite; a program needn't handle non-finite values.
Results may differ from the reference program's by a relative error of at most 0.0055.
Values may be sent and summed in bfloat16 or wider, within the bound.
No kernel may reach another device: no remote copies, remote signals or barrier semaphores. Data moves between devices by JAX's collectives and lax.ppermute only.
A program may use at most 128 MiB of HBM per device.

```python
import math
import jax
import jax.numpy as jnp
from jax import lax

D = 4096
QKW = 1024
VW = 2048
R = 512
TOKENS = 16384


def first_moment(key, rows, cols):
    row_scale = 0.3 * 10.0 ** (jnp.arange(rows, dtype=jnp.float32) / (rows - 1))
    col_scale = jnp.exp(jax.random.uniform(jax.random.fold_in(key, 7), (cols,), jnp.float32, -0.7, 0.7))
    base = jnp.clip(jax.random.normal(jax.random.fold_in(key, 11), (rows, cols), jnp.float32), -3.0, 3.0)
    return base * row_scale[:, None] * col_scale[None, :]


def draw_query_first(key, part):
    return first_moment(key, R, QKW)


def draw_output_first(key, part):
    return first_moment(key, R, D)


def level_of(stream_key, extent, split, low, high):
    def one(dim, blocks):
        heights = jax.random.uniform(jax.random.fold_in(jax.random.fold_in(stream_key, 6), dim), (blocks,), jnp.float32, low / len(split), high / len(split))
        return jnp.repeat(jnp.exp(heights), extent[dim] // blocks).reshape((-1,) + (1,) * (len(extent) - dim - 1))

    loudness = one(*split[0])
    for cut in split[1:]:
        loudness = loudness * one(*cut)
    return loudness


def scatter_about(stream_key, dims, spread, reach, shards=(), kind=jnp.bfloat16):
    result = spread * jax.random.normal(stream_key, dims, jnp.float32)
    if shards:
        result = result * level_of(stream_key, dims, shards, -0.22, 0.18)
    return jnp.clip(result, -reach, reach).astype(kind)


def setup_inputs(seed: int = 0) -> dict:
    keys = jax.random.split(jax.random.key(seed), 13)
    query_input = scatter_about(keys[0], (TOKENS, D), 1.0, 6.0, ((0, 16),))
    query_cotangent = scatter_about(keys[1], (TOKENS, QKW), (TOKENS ** -0.5), 0.046875, ((0, 16), (1, 2)))
    branch_output = scatter_about(keys[2], (TOKENS, VW), 1.0, 6.0, ((0, 16),))
    layer_cotangent = scatter_about(keys[3], (TOKENS, D), (TOKENS ** -0.5), 0.046875, ((0, 16), (1, 2)))
    query_weight = scatter_about(keys[4], (D, QKW), D ** -0.5, 0.09375, ((0, 16), (1, 2)), jnp.float32)
    output_weight = scatter_about(keys[5], (VW, D), VW ** -0.5, 0.125, ((0, 16), (1, 2)), jnp.float32)
    query_basis = scatter_about(keys[6], (D, R), D ** -0.5, 0.09375, ((0, 16),))
    output_basis = scatter_about(keys[7], (VW, R), VW ** -0.5, 0.125, ((0, 16),))
    query_first = draw_query_first(jax.random.fold_in(keys[12], 71), 0)
    query_second = jnp.clip(jnp.exp(math.log(2.0) - 2.0794415 * jax.random.uniform(keys[9], (R, QKW), jnp.float32) ** level_of(keys[9], (R, QKW), ((0, 16), (1, 2)), -0.2, 0.2)), 0.25, 2.0)
    output_first = draw_output_first(jax.random.fold_in(keys[12], 71), 0)
    output_second = jnp.clip(jnp.exp(math.log(2.0) - 2.0794415 * jax.random.uniform(keys[11], (R, D), jnp.float32) ** level_of(keys[11], (R, D), ((0, 16), (1, 2)), -0.2, 0.2)), 0.25, 2.0)
    return dict(query_input=query_input, query_cotangent=query_cotangent, branch_output=branch_output, layer_cotangent=layer_cotangent, query_weight=query_weight, output_weight=output_weight, query_basis=query_basis, output_basis=output_basis, query_first=query_first, query_second=query_second, output_first=output_first, output_second=output_second)


beta_first = 0.6
beta_second = 0.8
step_rate = 0.01
small_eps = 1e-06

def project(inputs, basis, cotangent):
    inner = jnp.dot(inputs.astype(jnp.float32), basis.astype(jnp.float32), precision=lax.Precision.HIGHEST, preferred_element_type=jnp.float32)
    return jnp.dot(inner.T, cotangent.astype(jnp.float32), precision=lax.Precision.HIGHEST, preferred_element_type=jnp.float32)

def advance(first, second, projected, basis, weight):
    first_next = beta_first * first + (1.0 - beta_first) * projected
    second_next = beta_second * second + (1.0 - beta_second) * projected * projected
    normed = first_next / jnp.sqrt(second_next)
    scale = lax.rsqrt(jnp.mean(normed * normed) + small_eps)
    rounded = normed.astype(jnp.bfloat16)
    update = scale * jnp.dot(basis.astype(jnp.float32), rounded.astype(jnp.float32), precision=lax.Precision.HIGHEST, preferred_element_type=jnp.float32)
    copy = (weight - step_rate * update).astype(jnp.bfloat16)
    return (update, first_next, second_next, copy)

def reference(query_input, query_cotangent, branch_output, layer_cotangent, query_weight, output_weight, query_basis, output_basis, query_first, query_second, output_first, output_second):
    projected_q = project(query_input, query_basis, query_cotangent)
    projected_o = project(branch_output, output_basis, layer_cotangent)
    update_q, first_q, second_q, copy_q = advance(query_first, query_second, projected_q, query_basis, query_weight)
    update_o, first_o, second_o, copy_o = advance(output_first, output_second, projected_o, output_basis, output_weight)
    return (update_q, update_o, first_q, second_q, first_o, second_o, copy_q, copy_o)
```

```python
import jax
import jax.numpy as jnp
from jax import lax
from jax.sharding import PartitionSpec as P


beta_first = 0.6
beta_second = 0.8
step_rate = 0.01
small_eps = 1e-06

f32 = jnp.float32
bf16 = jnp.bfloat16


def dot_rows(left, right):
    return lax.dot_general(left, right, (((0,), (0,)), ((), ())), preferred_element_type=f32)


def make_body(nf, nr, nt):
    assert nr == 4 and nt == 2

    def flip(value, bits):
        return lax.ppermute(value, "rep", [(k, k ^ bits) for k in range(nr)])

    def swap(value):
        return lax.ppermute(value, "tp", [(0, 1), (1, 0)])

    def shift(value, step):
        return lax.ppermute(value, "fs", [(k, (k + step) % nf) for k in range(nf)])

    def natural(blocks, place):
        rows = blocks[0].shape[0]
        whole = jnp.zeros((nf * rows, blocks[0].shape[1]), blocks[0].dtype)
        for s, block in enumerate(blocks):
            whole = lax.dynamic_update_slice(whole, block, ((place + nf - s) % nf * rows, 0))
        return whole

    def direct_gather(value, place):
        return natural([value] + [shift(value, s) for s in range(1, nf)], place)

    def ring_gather(value, place):
        blocks = [value]
        for _ in range(1, nf):
            blocks.append(shift(blocks[-1], 1))
        return natural(blocks, place)

    def body(
        query_input,
        query_cotangent,
        branch_output,
        layer_cotangent,
        query_weight,
        output_weight,
        query_basis,
        output_basis,
        query_first,
        query_second,
        output_first,
        output_second,
    ):
        place = lax.axis_index("fs")
        rep = lax.axis_index("rep")
        core = lax.axis_index("tp")
        low, high = rep % 2, rep // 2

        def kept_and_sent(own, other):
            mine = high == core
            return jnp.where(mine, own, other), jnp.where(mine, other, own)

        def relative(own, other):
            kept, sent = kept_and_sent(own, other)
            quarter = kept.shape[1] // 2
            rows = kept.shape[0]

            def part(value, bit):
                return lax.dynamic_slice(value, (0, bit * quarter), (rows, quarter))

            return [part(kept, low), part(kept, 1 - low), part(sent, low), part(sent, 1 - low)]

        def gather_basis(basis):
            half = basis.shape[1] // nt
            piece = lax.dynamic_slice(basis, (0, core * half), (basis.shape[0], half))
            block = direct_gather(piece, place)
            rows, split = block.shape[0], block.shape[0] // 2
            by_x, by_y = flip(block, 1), flip(block, 2)
            far = jnp.concatenate([flip(by_y[:split], 1), flip(by_x[split:], 2)], axis=0)
            whole = jnp.zeros((nr * rows, half), basis.dtype)
            for bits, value in enumerate((block, by_x, by_y, far)):
                whole = lax.dynamic_update_slice(whole, value, ((rep ^ bits) * rows, 0))
            return block, whole

        def project(inputs, whole, cotangent):
            inner = jnp.dot(inputs, whole, preferred_element_type=f32).astype(bf16)
            here, by_x, by_y, far = relative(inner, swap(inner))
            half = cotangent.shape[1] // 2
            left, right = cotangent[:, :half], cotangent[:, half:]
            block = here.shape[1]
            both = lambda a, b: jnp.concatenate([a, b], axis=1)
            got = flip(dot_rows(both(by_x, far), left).astype(bf16), 1)
            first = dot_rows(both(here, by_y), left) + got.astype(f32)
            got_other = flip(dot_rows(both(by_y, far), right).astype(bf16), 2)
            second = dot_rows(both(here, by_x), right) + got_other.astype(f32)
            first = first[:block] + flip(first[block:].astype(bf16), 2).astype(f32)
            second = second[:block] + flip(second[block:].astype(bf16), 1).astype(f32)
            total = jnp.concatenate([first, second], axis=1)
            rows = block // nf

            def rows_of(step):
                at = (place + step) % nf * rows
                return lax.dynamic_slice(total, (at, 0), (rows, total.shape[1]))

            arrived = [shift(rows_of(s).astype(bf16), s) for s in range(1, nf)]
            projected = rows_of(0)
            for value in arrived:
                projected = projected + value.astype(f32)
            return projected

        def moments(first, second, projected):
            first_next = beta_first * first + (1.0 - beta_first) * projected
            second_next = beta_second * second + (1.0 - beta_second) * projected * projected
            rounded = (first_next / jnp.sqrt(second_next)).astype(bf16)
            return first_next, second_next, rounded

        def spread(rounded):
            block = direct_gather(rounded, place)
            wide = block.astype(f32)
            total = jnp.sum(wide * wide).reshape(1, 1)
            total = total + swap(total)
            total = total + flip(total, 1)
            total = total + flip(total, 2)
            split = block.shape[1] // 2
            by_x, by_y = flip(block, 1), flip(block, 2)
            far = jnp.concatenate([flip(by_y[:, :split], 1), flip(by_x[:, split:], 2)], axis=1)
            return jnp.concatenate([block, by_x, by_y, far], axis=0), total[0, 0]

        def finish(basis_block, spread_rows, total, weights, rows):
            count = spread_rows.shape[0] * spread_rows.shape[1] * nt
            scale = lax.rsqrt(total / count + small_eps)
            basis_here = lax.dynamic_slice(basis_block, (place * rows, 0), (rows, basis_block.shape[1]))
            update = scale * jnp.dot(basis_here, spread_rows, preferred_element_type=f32)
            whole = scale * jnp.dot(basis_block, spread_rows, preferred_element_type=f32)
            return update, (weights.astype(f32) - step_rate * whole).astype(bf16)

        block_o, whole_o = gather_basis(output_basis)
        block_q, whole_q = gather_basis(query_basis)
        weights_o = ring_gather(output_weight.astype(bf16), place)
        weights_q = ring_gather(query_weight.astype(bf16), place)
        basis_o = jnp.concatenate(relative(block_o, swap(block_o)), axis=1)
        basis_q = jnp.concatenate(relative(block_q, swap(block_q)), axis=1)
        projected_o = project(branch_output, whole_o, layer_cotangent)
        projected_q = project(query_input, whole_q, query_cotangent)
        first_o, second_o, rounded_o = moments(output_first, output_second, projected_o)
        first_q, second_q, rounded_q = moments(query_first, query_second, projected_q)
        spread_o, total_o = spread(rounded_o)
        spread_q, total_q = spread(rounded_q)
        update_o, copy_o = finish(basis_o, spread_o, total_o, weights_o, output_basis.shape[0])
        update_q, copy_q = finish(basis_q, spread_q, total_q, weights_q, query_basis.shape[0])
        return (update_q, update_o, first_q, second_q, first_o, second_o, copy_q, copy_o)

    return body


def solution(mesh):
    tokens, columns = P(("fs", "rep"), None), P(("fs", "rep"), "tp")
    rows, both = P(("rep", "fs"), None), P(("rep", "fs"), "tp")
    in_specs = (tokens, columns, tokens, columns, both, both, rows, rows, both, both, both, both)
    out_specs = (both,) * 6 + (P("rep", "tp"),) * 2
    body = make_body(mesh.shape["fs"], mesh.shape["rep"], mesh.shape["tp"])
    return jax.shard_map(body, mesh=mesh, in_specs=in_specs, out_specs=out_specs, check_vma=False)
```

```python
import functools

import jax
import jax.numpy as jnp
from jax import lax
from jax.experimental import pallas as pl
from jax.experimental.pallas import tpu as pltpu
from jax.sharding import PartitionSpec as P


beta_first = 0.6
beta_second = 0.8
step_rate = 0.01
small_eps = 1e-06

f32 = jnp.float32
bf16 = jnp.bfloat16


def dot_rows(left, right):
    return lax.dot_general(left, right, (((0,), (0,)), ((), ())), preferred_element_type=f32)


def after(value, *others):
    return lax.optimization_barrier((value, *others))[0]


def finish_kernel(nf, nr, fold, rows, place_ref, scale_ref, basis_ref, *refs):
    pieces, weights = refs[: nr + 1], refs[nr + 1 : nr + 1 + nf]
    update_ref, copy_ref, spread_ref, product_ref = refs[nr + 1 + nf :]
    step, steps = pl.program_id(0), pl.num_programs(0)
    depth = pieces[0].shape[0]
    for k in range(nr - 1):
        spread_ref[k * depth : (k + 1) * depth, :] = pieces[k][...]

    @pl.when(step < steps // 2)
    def _():
        spread_ref[(nr - 1) * depth :, :] = pieces[nr - 1][...]

    @pl.when(step >= steps // 2)
    def _():
        spread_ref[(nr - 1) * depth :, :] = pieces[nr][...]

    product = jnp.dot(basis_ref[...], spread_ref[...], preferred_element_type=f32)
    product_ref[...] = scale_ref[0, 0] * product
    part = rows // fold
    for s in range(nf):
        source = lax.rem(place_ref[0] + (nf - s), nf)
        for n in range(fold):
            here = pl.ds(pl.multiple_of(source * rows + n * part, part), part)
            update = product_ref[here, :]
            weight = weights[s][:, n, :] if fold > 1 else weights[s][...]
            copy_ref[here, :] = (weight.astype(f32) - step_rate * update).astype(bf16)
    mine = pl.ds(pl.multiple_of(place_ref[0] * rows, rows), rows)
    update_ref[...] = product_ref[mine, :]


def finish(nf, nr, place, scale, basis, pieces, weights):
    depth, columns = pieces[0].shape
    rows = weights[0].shape[0]
    steps = 4 if columns % (4 * 256) == 0 else 2
    width = columns // steps
    half = steps // 2
    column = lambda s, p: (0, s)
    whole = lambda s, p: (0, 0)
    in_specs = [
        pl.BlockSpec((1, 1), whole, memory_space=pltpu.SMEM),
        pl.BlockSpec(basis.shape, whole),
        *[pl.BlockSpec((depth, width), column) for _ in range(nr - 1)],
        pl.BlockSpec((depth, width), lambda s, p: (0, jnp.minimum(s, half - 1))),
        pl.BlockSpec((depth, width), lambda s, p: (0, jnp.maximum(s - half, 0))),
        *[pl.BlockSpec((rows, width), column) for _ in weights],
    ]
    return pl.pallas_call(
        functools.partial(finish_kernel, nf, nr, 1, rows),
        grid_spec=pltpu.PrefetchScalarGridSpec(
            num_scalar_prefetch=1,
            grid=(steps,),
            in_specs=in_specs,
            out_specs=[
                pl.BlockSpec((rows, width), column),
                pl.BlockSpec((nf * rows, width), column),
            ],
            scratch_shapes=[
                pltpu.VMEM((nr * depth, width), bf16),
                pltpu.VMEM((nf * rows, width), f32),
            ],
        ),
        out_shape=[
            jax.ShapeDtypeStruct((rows, columns), f32),
            jax.ShapeDtypeStruct((nf * rows, columns), bf16),
        ],
    )(place.reshape(1), scale, basis, *pieces, *weights)


def make_body(nf, nr, nt):
    assert nr == 4 and nt == 2

    def flip(value, bits):
        return lax.ppermute(value, "rep", [(k, k ^ bits) for k in range(nr)])

    def swap(value):
        return lax.ppermute(value, "tp", [(0, 1), (1, 0)])

    def shift(value, step):
        return lax.ppermute(value, "fs", [(k, (k + step) % nf) for k in range(nf)])

    def body(
        query_input,
        query_cotangent,
        branch_output,
        layer_cotangent,
        query_weight,
        output_weight,
        query_basis,
        output_basis,
        query_first,
        query_second,
        output_first,
        output_second,
    ):
        place = lax.axis_index("fs")
        rep = lax.axis_index("rep")
        core = lax.axis_index("tp")
        low, high = rep % 2, rep // 2
        mine = high == core

        def natural(blocks):
            rows, columns = blocks[0].shape
            at = lax.broadcasted_iota(jnp.int32, (nf, 1, 1), 0)
            whole = jnp.broadcast_to(blocks[-1][None], (nf, rows, columns))
            for s in range(nf - 1):
                whole = jnp.where(at == (place + nf - s) % nf, blocks[s][None], whole)
            return whole.reshape(nf * rows, columns)

        def by_rep(blocks):
            rows, columns = blocks[0].shape
            whole = jnp.zeros((nr * rows, columns), blocks[0].dtype)
            for bits, value in enumerate(blocks):
                whole = lax.dynamic_update_slice(whole, value, ((rep ^ bits) * rows, 0))
            return whole

        def relative(own, other):
            kept, sent = jnp.where(mine, own, other), jnp.where(mine, other, own)
            quarter = kept.shape[1] // 2
            rows = kept.shape[0]

            def part(value, bit):
                return lax.dynamic_slice(value, (0, bit * quarter), (rows, quarter))

            return [part(kept, low), part(kept, 1 - low), part(sent, low), part(sent, 1 - low)]

        def half_basis(basis):
            half = basis.shape[1] // nt
            return lax.dynamic_slice(basis, (0, core * half), (basis.shape[0], half))

        def along_fs(value):
            return [value] + [shift(value, s) for s in range(1, nf)]

        def project(inner, other, cotangent):
            here, by_x, by_y, far = relative(inner, other)
            half = cotangent.shape[1] // 2
            left, right = cotangent[:, :half], cotangent[:, half:]
            block = here.shape[1]
            both = lambda a, b: jnp.concatenate([a, b], axis=1)
            got = flip(dot_rows(both(by_x, far), left).astype(bf16), 1)
            got_other = flip(dot_rows(both(by_y, far), right).astype(bf16), 2)
            first = dot_rows(both(here, by_y), left) + got.astype(f32)
            second = dot_rows(both(here, by_x), right) + got_other.astype(f32)
            first_more = flip(first[block:].astype(bf16), 2).astype(f32)
            second_more = flip(second[block:].astype(bf16), 1).astype(f32)
            first, second = first[:block] + first_more, second[:block] + second_more
            total = jnp.concatenate([first, second], axis=1)
            rows = block // nf

            def rows_of(step):
                at = (place + step) % nf * rows
                return lax.dynamic_slice(total, (at, 0), (rows, total.shape[1]))

            arrived = [shift(rows_of(s).astype(bf16), s) for s in range(1, nf)]
            projected = rows_of(0)
            for value in arrived:
                projected = projected + value.astype(f32)
            return projected

        def moments(first, second, projected):
            first_next = beta_first * first + (1.0 - beta_first) * projected
            second_next = beta_second * second + (1.0 - beta_second) * projected * projected
            rounded = (first_next / jnp.sqrt(second_next)).astype(bf16)
            return first_next, second_next, rounded

        def squares(block):
            wide = block.astype(f32)
            return jnp.sum(wide * wide).reshape(1, 1)

        basis_o = natural(along_fs(half_basis(output_basis)))
        basis_q = natural(along_fs(half_basis(query_basis)))
        others_o = [flip(basis_o, 1), flip(basis_o, 2), flip(basis_o, 3)]
        x_q, y_q = flip(basis_q, 1), flip(basis_q, 2)
        split = basis_q.shape[0] // 2
        far_q = [flip(y_q[:split], 1), flip(x_q[split:], 2)]
        whole_o = by_rep([basis_o, *others_o])
        whole_q = by_rep([basis_q, x_q, y_q, jnp.concatenate(far_q, axis=0)])

        fold = query_weight.shape[0] // output_weight.shape[0]
        rows_o, columns_o = output_weight.shape
        columns_q = query_weight.shape[1]
        packed = [output_weight] + [
            query_weight[n * rows_o : (n + 1) * rows_o] for n in range(fold)
        ]
        ring = [after(jnp.concatenate(packed, axis=1).astype(bf16), basis_q)]

        def turn():
            ring.append(shift(ring[-1], 1))

        inner_o = jnp.dot(branch_output, whole_o, preferred_element_type=f32).astype(bf16)
        other_o = swap(inner_o)
        projected_o = project(inner_o, other_o, layer_cotangent)
        inner_q = jnp.dot(query_input, whole_q, preferred_element_type=f32).astype(bf16)
        other_q = swap(inner_q)
        projected_q = project(inner_q, other_q, query_cotangent)
        late_o, late_q = lax.optimization_barrier((basis_o, basis_q, inner_q))[:2]
        order_o = jnp.concatenate(relative(late_o, swap(late_o)), axis=1)
        order_q = jnp.concatenate(relative(late_q, swap(late_q)), axis=1)

        first_o, second_o, rounded_o = moments(output_first, output_second, projected_o)
        first_q, second_q, rounded_q = moments(query_first, query_second, projected_q)
        block_o = natural(along_fs(rounded_o))
        block_q = natural(along_fs(rounded_q))

        for n in range(1, nf):
            if n == nf - 1:
                ring[-1] = after(ring[-1], block_o)
            turn()

        total = jnp.concatenate([squares(block_q), squares(block_o)], axis=1)
        total = total + swap(total)
        total = total + flip(total, 1)
        total = total + flip(total, 2)

        def spread(block, x, y):
            cut = block.shape[1] // 2
            return [block, x, y, flip(y[:, :cut], 1), flip(x[:, cut:], 2)]

        x_o, y_o = flip(block_o, 1), flip(block_o, 2)
        x_q, y_q = flip(block_q, 1), flip(block_q, 2)
        spread_o = spread(block_o, x_o, y_o)
        spread_q = spread(block_q, x_q, y_q)
        weights_o = [value[:, :columns_o] for value in ring]
        weights_q = [
            jnp.concatenate(
                [
                    value[:, columns_o + n * columns_q : columns_o + (n + 1) * columns_q]
                    for n in range(fold)
                ],
                axis=0,
            )
            for value in ring
        ]

        def end(total, order, pieces, weights):
            depth, columns = pieces[0].shape[0] * nr, pieces[0].shape[1]
            scale = lax.rsqrt(total / (depth * columns * nt) + small_eps)
            return finish(nf, nr, place, scale, order, pieces, weights)

        update_q, copy_q = end(total[:, :1], order_q, spread_q, weights_q)
        update_o, copy_o = end(total[:, 1:], order_o, spread_o, weights_o)
        return (update_q, update_o, first_q, second_q, first_o, second_o, copy_q, copy_o)

    return body


def solution(mesh):
    tokens, columns = P(("fs", "rep"), None), P(("fs", "rep"), "tp")
    rows, both = P(("rep", "fs"), None), P(("rep", "fs"), "tp")
    in_specs = (tokens, columns, tokens, columns, both, both, rows, rows, both, both, both, both)
    out_specs = (both,) * 6 + (P("rep", "tp"),) * 2
    nf = mesh.shape["fs"]
    body = make_body(nf, mesh.shape["rep"], mesh.shape["tp"])

    return jax.shard_map(body, mesh=mesh, in_specs=in_specs, out_specs=out_specs, check_vma=False)
```

```python
import functools

import jax
import jax.numpy as jnp
from jax import lax
from jax.experimental import pallas as pl
from jax.experimental.pallas import tpu as pltpu
from jax.sharding import PartitionSpec as P


beta_first = 0.6
beta_second = 0.8
step_rate = 0.01
small_eps = 1e-06

f32 = jnp.float32
bf16 = jnp.bfloat16
whole_vmem = pl.BlockSpec(memory_space=pltpu.VMEM)


def dot_rows(left, right):
    return lax.dot_general(left, right, (((0,), (0,)), ((), ())), preferred_element_type=f32)


def after(value, *others):
    return lax.optimization_barrier((value, *others))[0]


def natural_kernel(nf, squares, place_ref, *refs):
    blocks, refs = refs[:nf], refs[nf:]
    before, out_ref = refs[:-2] if squares else (), refs[-2 if squares else -1]
    rows = blocks[0].shape[0]
    for s in range(nf):
        source = lax.rem(place_ref[0] + (nf - s), nf)
        out_ref[pl.ds(pl.multiple_of(source * rows, rows), rows), :] = blocks[s][...]
    if squares:
        total = jnp.zeros((out_ref.shape[0], 128), f32)
        for at in range(0, out_ref.shape[1], 128):
            wide = out_ref[:, at : at + 128].astype(f32)
            total = total + wide * wide
        total = jnp.sum(total.reshape(-1, 8, 128), axis=0)
        refs[-1][...] = jnp.concatenate([part[...] for part in before] + [total], axis=0)


def natural(place, blocks, squares=False, before=()):
    nf = len(blocks)
    rows, columns = blocks[0].shape
    out_shape = [jax.ShapeDtypeStruct((nf * rows, columns), blocks[0].dtype)]
    if squares:
        out_shape.append(jax.ShapeDtypeStruct((8 * (len(before) + 1), 128), f32))
    out = pl.pallas_call(
        functools.partial(natural_kernel, nf, squares),
        in_specs=[pl.BlockSpec(memory_space=pltpu.SMEM)] + [whole_vmem] * (nf + len(before)),
        out_specs=[whole_vmem] * len(out_shape),
        out_shape=out_shape,
        compiler_params=pltpu.CompilerParams(vmem_limit_bytes=8 * 2**20),
    )(place.reshape(1), *blocks, *before)
    return out if squares else out[0]


def finish_kernel(nf, nr, fold, rows, count, first, place_ref, *refs):
    sums, basis_ref, refs = refs[:nr], refs[nr], refs[nr + 1 :]
    pieces, weights = refs[: nr + 1], refs[nr + 1 : nr + 1 + nf * fold]
    update_ref, copy_ref, spread_ref, product_ref = refs[nr + 1 + nf * fold :]
    step, steps = pl.program_id(0), pl.num_programs(0)
    depth = pieces[0].shape[0]
    for k in range(nr - 1):
        spread_ref[k * depth : (k + 1) * depth, :] = pieces[k][...]

    @pl.when(step < steps // 2)
    def _():
        spread_ref[(nr - 1) * depth :, :] = pieces[nr - 1][...]

    @pl.when(step >= steps // 2)
    def _():
        spread_ref[(nr - 1) * depth :, :] = pieces[nr][...]

    total = sum(part[first : first + 8, :] for part in sums)
    scale = lax.rsqrt(jnp.sum(total, keepdims=True) / count + small_eps)
    product = jnp.dot(basis_ref[...], spread_ref[...], preferred_element_type=f32)
    product_ref[...] = scale * product
    part = rows // fold
    for s in range(nf):
        source = lax.rem(place_ref[0] + (nf - s), nf)
        for n in range(fold):
            here = pl.ds(pl.multiple_of(source * rows + n * part, part), part)
            weight = weights[s * fold + n][...].astype(f32)
            copy_ref[here, :] = (weight - step_rate * product_ref[here, :]).astype(bf16)
    mine = pl.ds(pl.multiple_of(place_ref[0] * rows, rows), rows)
    update_ref[...] = product_ref[mine, :]


def finish(nf, nr, nt, place, sums, first, basis, pieces, ring, starts):
    depth, columns = pieces[0].shape
    part, fold = ring[0].shape[0], len(starts)
    rows = part * fold
    steps = 4 if columns % (4 * 256) == 0 else 2
    width = columns // steps
    half = steps // 2
    column = lambda s, p: (0, s)
    whole = lambda s, p: (0, 0)
    weight_specs = [
        pl.BlockSpec((part, width), lambda s, p, at=start // width: (0, at + s))
        for _ in ring
        for start in starts
    ]
    in_specs = [
        *[pl.BlockSpec(part.shape, whole) for part in sums],
        pl.BlockSpec(basis.shape, whole),
        *[pl.BlockSpec((depth, width), column) for _ in range(nr - 1)],
        pl.BlockSpec((depth, width), lambda s, p: (0, jnp.minimum(s, half - 1))),
        pl.BlockSpec((depth, width), lambda s, p: (0, jnp.maximum(s - half, 0))),
        *weight_specs,
    ]
    weights = [value for value in ring for _ in starts]
    return pl.pallas_call(
        functools.partial(finish_kernel, nf, nr, fold, rows, depth * nr * columns * nt, first),
        grid_spec=pltpu.PrefetchScalarGridSpec(
            num_scalar_prefetch=1,
            grid=(steps,),
            in_specs=in_specs,
            out_specs=[
                pl.BlockSpec((rows, width), column),
                pl.BlockSpec((nf * rows, width), column),
            ],
            scratch_shapes=[
                pltpu.VMEM((nr * depth, width), bf16),
                pltpu.VMEM((nf * rows, width), f32),
            ],
        ),
        out_shape=[
            jax.ShapeDtypeStruct((rows, columns), f32),
            jax.ShapeDtypeStruct((nf * rows, columns), bf16),
        ],
        compiler_params=pltpu.CompilerParams(vmem_limit_bytes=20 * 2**20),
    )(place.reshape(1), *sums, basis, *pieces, *weights)


def make_body(nf, nr, nt):
    assert nr == 4 and nt == 2

    def flip(value, bits):
        return lax.ppermute(value, "rep", [(k, k ^ bits) for k in range(nr)])

    def swap(value):
        return lax.ppermute(value, "tp", [(0, 1), (1, 0)])

    def shift(value, step):
        return lax.ppermute(value, "fs", [(k, (k + step) % nf) for k in range(nf)])

    def body(
        query_input,
        query_cotangent,
        branch_output,
        layer_cotangent,
        query_weight,
        output_weight,
        query_basis,
        output_basis,
        query_first,
        query_second,
        output_first,
        output_second,
    ):
        place = lax.axis_index("fs")
        rep = lax.axis_index("rep")
        core = lax.axis_index("tp")
        place, rep, core = lax.optimization_barrier((place, rep, core))
        low, high = rep % 2, rep // 2
        mine = high == core

        def relative(own, other):
            kept, sent = lax.select_n(mine, other, own), lax.select_n(mine, own, other)
            quarter = kept.shape[1] // 2
            rows = kept.shape[0]

            def part(value, bit):
                return lax.dynamic_slice(value, (0, bit * quarter), (rows, quarter))

            return [part(kept, low), part(kept, 1 - low), part(sent, low), part(sent, 1 - low)]

        def half_basis(basis):
            half = basis.shape[1] // nt
            return lax.dynamic_slice(basis, (0, core * half), (basis.shape[0], half))

        def along_fs(value):
            return [value] + [shift(value, s) for s in range(1, nf)]

        def sum_blocks(inputs, blocks):
            width = inputs.shape[1] // nr
            total = None
            for bits, pieces in blocks:
                at = (rep ^ bits) * width
                for piece in pieces:
                    depth = piece.shape[0]
                    columns = lax.dynamic_slice(inputs, (0, at), (inputs.shape[0], depth))
                    more = jnp.dot(columns, piece, preferred_element_type=f32)
                    total = more if total is None else total + more
                    at = at + depth
            return total.astype(bf16)

        def project(inner, other, cotangent):
            here, by_x, by_y, far = relative(inner, other)
            half = cotangent.shape[1] // 2
            left, right = cotangent[:, :half], cotangent[:, half:]
            block = here.shape[1]
            both = lambda a, b: jnp.concatenate([a, b], axis=1)
            sent = dot_rows(both(by_x, far), left).astype(bf16)
            sent_other = dot_rows(both(by_y, far), right).astype(bf16)
            got = flip(sent, 1).astype(f32)
            got_other = flip(sent_other, 2).astype(f32)
            first_on = (dot_rows(by_y, left) + got[block:]).astype(bf16)
            second_on = (dot_rows(by_x, right) + got_other[block:]).astype(bf16)
            first_more = flip(first_on, 2).astype(f32)
            second_more = flip(second_on, 1).astype(f32)
            first = dot_rows(here, left) + got[:block] + first_more
            second = dot_rows(here, right) + got_other[:block] + second_more
            total = jnp.concatenate([first, second], axis=1)
            rows = block // nf

            def rows_of(step):
                at = (place + step) % nf * rows
                return lax.dynamic_slice(total, (at, 0), (rows, total.shape[1]))

            arrived = [shift(rows_of(s).astype(bf16), s) for s in range(1, nf)]
            projected = rows_of(0)
            for value in arrived:
                projected = projected + value.astype(f32)
            return projected, sent_other, second_on

        def moments(first, second, projected):
            first_next = beta_first * first + (1.0 - beta_first) * projected
            second_next = beta_second * second + (1.0 - beta_second) * projected * projected
            rounded = (first_next / jnp.sqrt(second_next)).astype(bf16)
            return first_next, second_next, rounded

        basis_o = natural(place, along_fs(half_basis(output_basis)))
        basis_q = natural(place, along_fs(half_basis(query_basis)))
        x_o, y_o, d_o = flip(basis_o, 1), flip(basis_o, 2), flip(basis_o, 3)
        x_q, y_q = flip(basis_q, 1), flip(basis_q, 2)
        inner_o = sum_blocks(branch_output, [(0, [basis_o]), (1, [x_o]), (2, [y_o]), (3, [d_o])])
        projected_o, sent_o, on_o = project(inner_o, swap(inner_o), layer_cotangent)
        x_q, y_q = lax.optimization_barrier((x_q, y_q, sent_o))[:2]
        split = basis_q.shape[0] // 2
        far_q = [flip(y_q[:split], 1), flip(x_q[split:], 2)]
        far_q = lax.optimization_barrier((*far_q, on_o))[:2]
        inner_q = sum_blocks(query_input, [(0, [basis_q]), (1, [x_q]), (2, [y_q]), (3, far_q)])
        projected_q = project(inner_q, swap(inner_q), query_cotangent)[0]

        fold = query_weight.shape[0] // output_weight.shape[0]
        rows_o, columns_o = output_weight.shape
        columns_q = query_weight.shape[1]
        packed = [output_weight] + [
            query_weight[n * rows_o : (n + 1) * rows_o] for n in range(fold)
        ]
        ring = [after(jnp.concatenate(packed, axis=1).astype(bf16), basis_q)]

        def turn():
            ring.append(shift(ring[-1], 1))

        late_o, late_q = lax.optimization_barrier((basis_o, basis_q, inner_q))[:2]
        order_o = jnp.concatenate(relative(late_o, swap(late_o)), axis=1)
        order_q = jnp.concatenate(relative(late_q, swap(late_q)), axis=1)

        first_o, second_o, rounded_o = moments(output_first, output_second, projected_o)
        first_q, second_q, rounded_q = moments(query_first, query_second, projected_q)
        block_o, sums_o = natural(place, along_fs(rounded_o), True)
        blocks_q = lax.optimization_barrier((*along_fs(rounded_q), block_o))[:-1]
        block_q, sums = natural(place, blocks_q, True, (sums_o,))

        for n in range(1, nf):
            if n == nf - 1:
                ring[-1] = after(ring[-1], block_o)
            turn()

        sums = sums + swap(sums)
        sums = [sums, flip(sums, 1), flip(sums, 2), flip(sums, 3)]

        def spread(block, x, y):
            cut = block.shape[1] // 2
            return [block, x, y, flip(y[:, :cut], 1), flip(x[:, cut:], 2)]

        x_o, y_o = flip(block_o, 1), flip(block_o, 2)
        x_q, y_q = flip(block_q, 1), flip(block_q, 2)
        spread_o = spread(block_o, x_o, y_o)
        spread_q = spread(block_q, x_q, y_q)
        starts_q = [columns_o + n * columns_q for n in range(fold)]

        def end(first, order, pieces, starts):
            return finish(nf, nr, nt, place, sums, first, order, pieces, ring, starts)

        update_q, copy_q = end(8, order_q, spread_q, starts_q)
        update_o, copy_o = end(0, order_o, spread_o, [0])
        return (update_q, update_o, first_q, second_q, first_o, second_o, copy_q, copy_o)

    return body


def solution(mesh):
    tokens, columns = P(("fs", "rep"), None), P(("fs", "rep"), "tp")
    rows, both = P(("rep", "fs"), None), P(("rep", "fs"), "tp")
    in_specs = (tokens, columns, tokens, columns, both, both, rows, rows, both, both, both, both)
    out_specs = (both,) * 6 + (P("rep", "tp"),) * 2
    nf = mesh.shape["fs"]
    body = make_body(nf, mesh.shape["rep"], mesh.shape["tp"])

    return jax.shard_map(body, mesh=mesh, in_specs=in_specs, out_specs=out_specs, check_vma=False)
```
